32 devices in a mesh: gr: 2 (over x), sp: 8 (over z, y), tp: 2 (over core).
Axes of the slice: x: 2, y: 2, z: 4, core: 2. Of those that a mesh axis runs over, the one named last changes fastest.
Arguments:
- tokens: bfloat16 [4, 2, 2048, 4096], P('gr', 'tp', 'sp'), may hold values from -6 to 6
- ln_gain: bfloat16 [4096], replicated, may hold values from 0.099609375 to 1.8984375
- w_key: bfloat16 [4096, 256], P('sp'), may hold values from -0.09375 to 0.09375
- w_value: bfloat16 [4096, 256], P('sp'), may hold values from -0.09375 to 0.09375
- queries: bfloat16 [16, 512], P(('gr', 'sp')), may hold values from -6 to 6
- head_shift: float32 [4, 8], replicated
- key_shift: float32 [16, 4096], P(('gr', 'sp'), 'tp')
Outputs:
- kv_cache: bfloat16 [16, 4096, 128], P(('gr', 'sp'), 'tp')
- first_read: float32 [16, 512], P(('gr', 'sp'))
The draws below stay inside these ranges and needn't reach their ends.
All inputs are finite; a program needn't handle non-finite values.
Results may differ from the reference program's by a relative error of at most 0.0064.
Values may be sent and summed in bfloat16 or wider, within the bound.
A program may use at most 64 MiB of HBM per device.

```python
import math
import jax
import jax.numpy as jnp
from jax import lax

D = 4096
HD = 64
KVH = 4
GROUP = 8
SEQS = 4
SECTIONS = 2
SPAN = 2048
LEN = 4096
PAIRS = 16


def draw_head_shift(key, part):
    first, second, third = jax.random.split(key, 3)
    fast_share = 0.5
    picker = jax.random.uniform(first, (KVH, GROUP), jnp.float32)
    fast_value = jax.random.uniform(second, (KVH, GROUP), jnp.float32, -4.5, -3.5)
    slow_value = -math.log(LEN) - 1.5 + jax.random.uniform(third, (KVH, GROUP), jnp.float32, -0.3, 0.3)
    return jnp.where(picker < fast_share, fast_value, slow_value)


def draw_key_shift(key, part):
    first, second, third, fourth = jax.random.split(key, 4)
    spread = 0.7
    section_level = jax.random.uniform(first, (PAIRS, SECTIONS), jnp.float32, -spread, spread)
    section_full = jnp.repeat(section_level, SPAN, axis=1)
    rough = jax.random.uniform(second, (PAIRS, LEN), jnp.float32, -0.5, 0.5)
    places = jax.random.randint(third, (PAIRS, 4), 0, LEN)
    marks = jnp.any(jnp.arange(LEN)[None, None, :] == places[:, :, None], axis=1)
    height = math.log(LEN) + 0.5 + jax.random.uniform(fourth, (PAIRS, LEN), jnp.float32, -0.3, 0.3)
    return section_full + rough + jnp.where(marks, height, 0.0)


def levels(key, extent, cuts, smallest, top_value):
    level = 1.0
    for dim, blocks in cuts:
        heights = jax.random.uniform(jax.random.fold_in(jax.random.fold_in(key, 6), dim), (blocks,), jnp.float32, smallest / len(cuts), top_value / len(cuts))
        level = level * jnp.repeat(jnp.exp(heights), extent[dim] // blocks).reshape((-1,) + (1,) * (len(extent) - 1 - dim))
    return level


def bell_draw(rng, shape, deviation, most, cuts=(), kind=jnp.bfloat16):
    values = jax.random.normal(rng, shape, jnp.float32) * deviation
    if len(cuts) > 0:
        values = levels(rng, shape, cuts, -0.22, 0.18) * values
    return jnp.clip(values, min=-most, max=most).astype(kind)


def setup_inputs(seed: int = 0) -> dict:
    splits = jax.random.split(jax.random.key(seed), 8)
    tokens = bell_draw(splits[0], (SEQS, SECTIONS, SPAN, D), 1.0, 6.0, ((0, 2), (1, 2), (2, 8)))
    ln_gain = jnp.clip(1.0 + 0.18 * jax.random.normal(splits[1], (D,), jnp.float32), 0.099609375, 1.8984375).astype(jnp.bfloat16)
    w_key = bell_draw(splits[2], (D, KVH * HD), D ** -0.5, 0.09375, ((0, 8),))
    w_value = bell_draw(splits[3], (D, KVH * HD), D ** -0.5, 0.09375, ((0, 8),))
    queries = bell_draw(splits[4], (PAIRS, GROUP * HD), 1.0, 6.0, ((0, 16),))
    head_shift = draw_head_shift(jax.random.fold_in(splits[7], 71), 0)
    key_shift = draw_key_shift(jax.random.fold_in(splits[7], 71), 0)
    return {"tokens": tokens, "ln_gain": ln_gain, "w_key": w_key, "w_value": w_value, "queries": queries, "head_shift": head_shift, "key_shift": key_shift}


epsilon = 1e-05

def project_sequence(block, ln_gain, w_key, w_value):
    flat_rows = block.reshape(LEN, D).astype(jnp.float32)
    row_mean = lax.optimization_barrier(jnp.mean(flat_rows, axis=1, keepdims=True))
    centred = flat_rows - row_mean
    row_var = lax.optimization_barrier(jnp.mean(centred * centred, axis=1, keepdims=True))
    normed = (centred * lax.rsqrt(row_var + epsilon) * ln_gain.astype(jnp.float32)).astype(jnp.bfloat16)
    keys = jnp.dot(normed, w_key, preferred_element_type=jnp.float32).astype(jnp.bfloat16)
    values = jnp.dot(normed, w_value, preferred_element_type=jnp.float32).astype(jnp.bfloat16)
    joined = jnp.concatenate([keys.reshape(LEN, KVH, HD), values.reshape(LEN, KVH, HD)], axis=2)
    return jnp.transpose(joined, (1, 0, 2))

def read_pair(pair_cache, query, shift_row, head_row):
    keys = pair_cache[:, :HD]
    values = pair_cache[:, HD:]
    logits = jnp.dot(query.reshape(GROUP, HD), keys.T, preferred_element_type=jnp.float32) * HD ** (-0.5)
    logits = logits + head_row[:, None] + shift_row[None, :]
    log_beta = jax.nn.log_sigmoid(logits)
    log_keep = (log_beta - logits).reshape(GROUP, SECTIONS, SPAN)
    within = lax.cumsum(log_keep, axis=2, reverse=True) - log_keep
    local_weight = jnp.exp(log_beta.reshape(GROUP, SECTIONS, SPAN) + within).astype(jnp.bfloat16)
    parts = jnp.einsum('gsj,sjd->gsd', local_weight.astype(jnp.float32), values.reshape(SECTIONS, SPAN, HD).astype(jnp.float32))
    totals = lax.optimization_barrier(jnp.sum(log_keep, axis=2))
    carry = lax.cumsum(totals, axis=1, reverse=True) - totals
    return lax.optimization_barrier(jnp.sum(jnp.exp(carry)[:, :, None] * parts, axis=1)).reshape(GROUP * HD)

def reference(tokens, ln_gain, w_key, w_value, queries, head_shift, key_shift):
    caches = lax.map(lambda block: project_sequence(block, ln_gain, w_key, w_value), tokens)
    kv_cache = caches.reshape(PAIRS, LEN, 2 * HD)
    head_rows = jnp.tile(head_shift, (SEQS, 1))
    first_read = lax.map(lambda items: read_pair(items[0], items[1], items[2], items[3]), (kv_cache, queries, key_shift, head_rows))
    return (kv_cache, first_read)
```

```python
import functools

import jax
import jax.numpy as jnp
from jax import lax
from jax.experimental import pallas as pl
from jax.experimental.pallas import tpu as pltpu
from jax.sharding import PartitionSpec as P

epsilon = 1e-05
STAGES = 4
MESH = pl.DeviceIdType.MESH


def layout(mesh):
    sp, gr, tp = mesh.shape["sp"], mesh.shape["gr"], mesh.shape["tp"]
    inner = 1
    while inner * inner * 4 <= sp and sp % (inner * 2) == 0:
        inner *= 2
    return sp // inner, inner, gr, tp


def body(
    grid, head_size,
    tokens, gain, w_key, w_value, queries, head_shift, key_shift,
    cache, read,
    raw, normed, weights, acc, outgoing, incoming, totals, parts,
    send_sem, recv_sem, load_sem,
):
    depth, inner, groups, sections = grid
    seats = depth * inner
    seat, group, section = lax.axis_index("sp"), lax.axis_index("gr"), lax.axis_index("tp")
    lane, place = seat // inner, seat % inner
    rows, width = raw.shape
    shard, columns = w_key.shape
    piece = shard // (groups * sections)
    kv_heads, heads = head_shift.shape
    seqs = seats // kv_heads
    sub = rows // seqs
    half = sub // 2
    stage_rows = rows // STAGES

    sent = []

    def push(source, target, **where):
        at = len(sent)
        copy = pltpu.make_async_remote_copy(
            src_ref=source, dst_ref=target, send_sem=send_sem.at[at], recv_sem=recv_sem.at[at],
            device_id=where, device_id_type=MESH,
        )
        copy.start()
        sent.append(copy)
        return copy

    own = pl.ds(pl.multiple_of(seat * shard, shard), shard)
    loads = []
    for at, source in enumerate((w_key, w_value)):
        loads.append(pltpu.make_async_copy(source, weights.at[at, own], load_sem.at[at]))
        loads[-1].start()
    fills = []
    for at in range(STAGES):
        block = pl.ds(at * stage_rows, stage_rows)
        fills.append(pltpu.make_async_copy(tokens.at[block], raw.at[block], load_sem.at[2 + at]))
        fills[-1].start()

    def seat_at(k, j):
        return lax.rem(lane + depth - k, depth) * inner + lax.rem(place + inner - j, inner)

    barrier = pltpu.get_barrier_semaphore()
    for i in range(1, seats):
        pl.semaphore_signal(barrier, 1, device_id={"sp": lax.rem(seat + i, seats)}, device_id_type=MESH)
    for i in range(1, groups):
        pl.semaphore_signal(barrier, 1, device_id={"gr": lax.rem(group + i, groups)}, device_id_type=MESH)
    for i in range(1, sections):
        pl.semaphore_signal(barrier, 1, device_id={"tp": lax.rem(section + i, sections)}, device_id_type=MESH)
    pl.semaphore_wait(barrier, seats + groups + sections - 3)

    def block_of(m, k, j, g):
        share = lax.rem(group + groups - g, groups) * sections + section
        start = seat_at(k, j) * shard + share * piece
        return weights.at[m, pl.ds(pl.multiple_of(start, piece), piece)]

    got = {}
    crossed = {}

    def along_lane(m):
        for k in range(1, depth):
            to = lax.rem(lane + k, depth) * inner + place
            block = block_of(m, 0, 0, 0)
            got[m, k, 0, 0] = push(block, block, sp=to)

    def along_place(m, k, g):
        for j in range(1, inner):
            to = lane * inner + lax.rem(place + j, inner)
            block = block_of(m, k, 0, g)
            got[m, k, j, g] = push(block, block, sp=to)

    def along_group(m, k, j):
        if k == 0 and j == 0:
            return
        for g in range(1, groups):
            block = block_of(m, k, j, 0)
            got[m, k, j, g] = push(block, block, gr=lax.rem(group + g, groups))

    def along_section(m, k, j, g):
        if k == 0 and j == 0:
            return
        block = block_of(m, k, j, g)
        for t in range(1, sections):
            copy = push(block, block, tp=lax.rem(section + t, sections))
            crossed.setdefault((m, k), []).append(copy)

    def normalise(at):
        fills[at].wait()
        step = 32

        @pl.loop(0, stage_rows // step)
        def _(i):
            here = pl.ds(pl.multiple_of(at * stage_rows + i * step, step), step)
            x = raw[here, :].astype(jnp.float32)
            mean = jnp.mean(x, axis=1, keepdims=True)
            centred = x - mean
            var = jnp.mean(centred * centred, axis=1, keepdims=True)
            scale = gain[...].astype(jnp.float32)
            normed[here, :] = (centred * lax.rsqrt(var + epsilon) * scale).astype(jnp.bfloat16)

    def multiply(m, k):
        for copy in crossed.get((m, k), ()):
            copy.wait_recv()
        span = inner * shard
        start = pl.multiple_of(lax.rem(lane + depth - k, depth) * span, span)
        out = jnp.dot(normed[:, pl.ds(start, span)], weights[m, pl.ds(start, span), :], preferred_element_type=jnp.float32)
        if k == 0:
            acc[...] = out
        else:
            acc[...] += out

    swapped = {}

    def exchange(m):
        for pair in range(seats):
            seq, head = pair // kv_heads, pair % kv_heads
            cut = slice(head * head_size, (head + 1) * head_size)
            first = acc[seq * sub:seq * sub + half, cut]
            second = acc[seq * sub + half:(seq + 1) * sub, cut]
            outgoing[m, pair] = jnp.concatenate([first, second], axis=1).astype(jnp.bfloat16)
        for i in range(1, seats):
            to = lax.rem(seat + i, seats)
            swapped[m, i] = push(outgoing.at[m, to], incoming.at[m, seat], sp=to)
        incoming[m, pl.ds(seat, 1)] = outgoing[m, pl.ds(seat, 1)]

    loads[0].wait()
    along_place(0, 0, 0)
    along_lane(0)
    loads[1].wait()
    along_lane(1)
    for g in range(groups):
        along_place(1, 0, g)
    normalise(0)
    for j in range(1, inner):
        got[0, 0, j, 0].wait_recv()
        along_group(0, 0, j)
        along_section(0, 0, j, 0)
    normalise(1)
    for k in range(1, depth):
        got[0, k, 0, 0].wait_recv()
        along_place(0, k, 0)
        along_group(0, k, 0)
        along_section(0, k, 0, 0)
        got[1, k, 0, 0].wait_recv()
        along_group(1, k, 0)
        along_place(1, k, 0)
        along_section(1, k, 0, 0)
        if k == 1:
            normalise(2)
    for k in range(1, depth):
        for j in range(1, inner):
            got[0, k, j, 0].wait_recv()
            along_group(0, k, j)
            along_section(0, k, j, 0)
        for g in range(1, groups):
            got[1, k, 0, g].wait_recv()
            along_place(1, k, g)
            along_section(1, k, 0, g)
    for at in range(3, STAGES):
        normalise(at)
    for m in range(2):
        for k in range(depth):
            for j in range(inner):
                for g in range(groups):
                    last = g > 0 if m == 0 else j > 0
                    if last and not (k == 0 and j == 0):
                        got[m, k, j, g].wait_recv()
                        along_section(m, k, j, g)
            if k > 0:
                multiply(m, k - 1)
        multiply(m, depth - 1)
        exchange(m)

    query = queries[...].astype(jnp.float32)
    query = jnp.concatenate([query[:, g * head_size:(g + 1) * head_size] for g in range(heads)], axis=0)
    blank = jnp.zeros_like(query)
    query = jnp.concatenate(
        [jnp.concatenate([query, blank], axis=1), jnp.concatenate([blank, query], axis=1)], axis=0
    ).astype(jnp.bfloat16)
    mine = lax.broadcasted_iota(jnp.int32, (kv_heads, heads), 0) == lax.rem(seat, kv_heads)
    shift = jnp.sum(jnp.where(mine, head_shift[...], 0.0), axis=0, keepdims=True)
    eye = lax.broadcasted_iota(jnp.int32, (heads, heads), 0) == lax.broadcasted_iota(jnp.int32, (heads, heads), 1)
    shift = jnp.sum(jnp.where(eye, jnp.broadcast_to(shift, (heads, heads)), 0.0), axis=1, keepdims=True)
    later = (
        lax.broadcasted_iota(jnp.int32, (half, half), 0) > lax.broadcasted_iota(jnp.int32, (half, half), 1)
    ).astype(jnp.float32)

    for i in range(1, seats):
        swapped[0, i].wait_recv()
    keys = incoming[0].reshape(seats * half, 2 * head_size)
    logits = lax.dot_general(query, keys, (((1,), (1,)), ((), ())), preferred_element_type=jnp.float32)
    logits = logits * head_size ** (-0.5)
    betas, keeps = [], []
    for at in range(2 * seats):
        q, h = at // 2, at % 2
        z = logits[h * heads:(h + 1) * heads, q * half:(q + 1) * half]
        z = z + shift + key_shift[:, at * half:(at + 1) * half]
        tail = jnp.log1p(jnp.exp(-jnp.abs(z)))
        betas.append(jnp.minimum(z, 0.0) - tail)
        keeps.append(jnp.minimum(-z, 0.0) - tail)
    within = jnp.dot(
        jnp.concatenate(keeps, axis=0), later, preferred_element_type=jnp.float32, precision=lax.Precision.HIGHEST
    )
    running = jnp.zeros((heads, 1), jnp.float32)
    local = [None] * (2 * seats)
    for at in reversed(range(2 * seats)):
        local[at] = jnp.exp(betas[at] + within[at * heads:(at + 1) * heads] + running)
        running = running + jnp.sum(keeps[at], axis=1, keepdims=True)
    local = jnp.concatenate(
        [jnp.concatenate(local[0::2], axis=1), jnp.concatenate(local[1::2], axis=1)], axis=0
    ).astype(jnp.bfloat16)
    totals[section] = jnp.broadcast_to(running, totals.shape[1:])
    arrivals = [
        push(totals.at[section], totals.at[section], tp=lax.rem(section + t, sections)) for t in range(1, sections)
    ]
    for copy in arrivals:
        copy.wait_recv()
    carry = jnp.zeros((heads, head_size), jnp.float32)
    for t in reversed(range(sections)):
        carry = carry + jnp.where(section < t, totals[t][:, :head_size], 0.0)
    carry = jnp.exp(carry)

    for i in range(1, seats):
        swapped[1, i].wait_recv()
    values = incoming[1].reshape(seats * half, 2 * head_size)
    part = jnp.dot(local, values, preferred_element_type=jnp.float32)
    part = carry * (part[:heads, :head_size] + part[heads:, head_size:])
    parts[section] = jnp.concatenate([part, part], axis=1)
    arrivals = [
        push(parts.at[section], parts.at[section], tp=lax.rem(section + t, sections)) for t in range(1, sections)
    ]
    for q in range(seats):
        for h in range(2):
            cut = slice(h * head_size, (h + 1) * head_size)
            start = (2 * q + h) * half
            cache[0, start:start + half, :] = jnp.concatenate([incoming[0, q][:, cut], incoming[1, q][:, cut]], axis=1)
    for copy in arrivals:
        copy.wait_recv()
    total = parts[0]
    for t in range(1, sections):
        total = total + parts[t]
    for g in range(heads):
        read[:, g * head_size:(g + 1) * head_size] = total[g:g + 1, :head_size]
    for copy in sent:
        copy.wait_send()


def copies(grid):
    depth, inner, groups, sections = grid
    pieces = depth * inner * groups
    gather = pieces + (pieces - groups) * (sections - 1)
    return 2 * gather + 2 * (depth * inner - 1) + 2 * (sections - 1)


def local(grid, tokens, ln_gain, w_key, w_value, queries, head_shift, key_shift):
    depth, inner, groups, sections = grid
    seats = depth * inner
    seqs, _, sub, width = tokens.shape
    rows = seqs * sub
    columns = w_key.shape[1]
    kv_heads, heads = head_shift.shape
    head_size = columns // kv_heads
    vmem = pl.BlockSpec(memory_space=pltpu.VMEM)
    hbm = pl.BlockSpec(memory_space=pl.ANY)
    count = copies(grid)
    cache, read = pl.pallas_call(
        functools.partial(body, grid, head_size),
        out_shape=(
            jax.ShapeDtypeStruct((1, seats * sub, 2 * head_size), jnp.bfloat16),
            jax.ShapeDtypeStruct((1, heads * head_size), jnp.float32),
        ),
        in_specs=[hbm, vmem, hbm, hbm, vmem, vmem, vmem],
        out_specs=(vmem, vmem),
        scratch_shapes=[
            pltpu.VMEM((rows, width), jnp.bfloat16),
            pltpu.VMEM((rows, width), jnp.bfloat16),
            pltpu.VMEM((2, width, columns), jnp.bfloat16),
            pltpu.VMEM((rows, columns), jnp.float32),
            pltpu.VMEM((2, seats, sub // 2, 2 * head_size), jnp.bfloat16),
            pltpu.VMEM((2, seats, sub // 2, 2 * head_size), jnp.bfloat16),
            pltpu.VMEM((sections, heads, 2 * head_size), jnp.float32),
            pltpu.VMEM((sections, heads, 2 * head_size), jnp.float32),
            pltpu.SemaphoreType.DMA((count,)),
            pltpu.SemaphoreType.DMA((count,)),
            pltpu.SemaphoreType.DMA((2 + STAGES,)),
        ],
        compiler_params=pltpu.CompilerParams(
            collective_id=0, has_side_effects=True, vmem_limit_bytes=60 * 1024 * 1024
        ),
    )(tokens.reshape(rows, width), ln_gain.reshape(1, width), w_key, w_value, queries, head_shift, key_shift)
    return cache, read


def solution(mesh):
    in_specs = (
        P("gr", "tp", "sp", None),
        P(),
        P("sp", None),
        P("sp", None),
        P(("gr", "sp"), None),
        P(),
        P(("gr", "sp"), "tp"),
    )
    out_specs = (P(("gr", "sp"), "tp", None), P(("gr", "sp"), None))
    return jax.shard_map(
        functools.partial(local, layout(mesh)), mesh=mesh, in_specs=in_specs, out_specs=out_specs, check_vma=False
    )
```

```python
import functools

import jax
import jax.numpy as jnp
from jax import lax
from jax.experimental import pallas as pl
from jax.experimental.pallas import tpu as pltpu
from jax.sharding import PartitionSpec as P

epsilon = 1e-05
STAGES = 4
NORM_AT = (0.5, 2.6, 3.1, 5.1)
LAG, LANE, HOP, CROSS = 3.0, 1.0, 2.5, 1.0
ORDERS = ((0, 0, 0, 0), (1, 1, 1, 1))
MESH = pl.DeviceIdType.MESH


def layout(mesh):
    sp, gr, tp = mesh.shape["sp"], mesh.shape["gr"], mesh.shape["tp"]
    inner = 1
    while inner * inner * 4 <= sp and sp % (inner * 2) == 0:
        inner *= 2
    return sp // inner, inner, gr, tp


def body(
    grid, head_size,
    tokens, gain, w_key, w_value, queries, head_shift, key_shift,
    cache, read,
    raw, normed, weights, acc, outgoing, incoming, totals, parts,
    send_sem, recv_sem, load_sem,
):
    depth, inner, groups, sections = grid
    seats = depth * inner
    seat, group, section = lax.axis_index("sp"), lax.axis_index("gr"), lax.axis_index("tp")
    lane, place = seat // inner, seat % inner
    rows, width = raw.shape
    shard, columns = w_key.shape
    piece = shard // (groups * sections)
    kv_heads, heads = head_shift.shape
    seqs = seats // kv_heads
    sub = rows // seqs
    half = sub // 2
    stage_rows = rows // STAGES

    sent = []

    def push(source, target, **where):
        at = len(sent)
        copy = pltpu.make_async_remote_copy(
            src_ref=source, dst_ref=target, send_sem=send_sem.at[at], recv_sem=recv_sem.at[at],
            device_id=where, device_id_type=MESH,
        )
        copy.start()
        sent.append(copy)
        return copy

    own = pl.ds(pl.multiple_of(seat * shard, shard), shard)
    loads = []
    for at, source in enumerate((w_key, w_value)):
        loads.append(pltpu.make_async_copy(source, weights.at[at, own], load_sem.at[at]))
        loads[-1].start()
    fills = []
    for at in range(STAGES):
        block = pl.ds(at * stage_rows, stage_rows)
        fills.append(pltpu.make_async_copy(tokens.at[block], raw.at[block], load_sem.at[2 + at]))
        fills[-1].start()

    def seat_at(k, j):
        return lax.rem(lane + depth - k, depth) * inner + lax.rem(place + inner - j, inner)

    barrier = pltpu.get_barrier_semaphore()
    for i in range(1, seats):
        pl.semaphore_signal(barrier, 1, device_id={"sp": lax.rem(seat + i, seats)}, device_id_type=MESH)
    for i in range(1, groups):
        pl.semaphore_signal(barrier, 1, device_id={"gr": lax.rem(group + i, groups)}, device_id_type=MESH)
    for i in range(1, sections):
        pl.semaphore_signal(barrier, 1, device_id={"tp": lax.rem(section + i, sections)}, device_id_type=MESH)
    pl.semaphore_wait(barrier, seats + groups + sections - 3)

    def block_of(m, k, j, g):
        share = lax.rem(group + groups - g, groups) * sections + section
        start = seat_at(k, j) * shard + share * piece
        return weights.at[m, pl.ds(pl.multiple_of(start, piece), piece)]

    got = {}
    crossed = {}

    def along_lane(m):
        for k in range(1, depth):
            to = lax.rem(lane + k, depth) * inner + place
            block = block_of(m, 0, 0, 0)
            got[m, k, 0, 0] = push(block, block, sp=to)

    def along_place(m, k, g):
        for j in range(1, inner):
            to = lane * inner + lax.rem(place + j, inner)
            block = block_of(m, k, 0, g)
            got[m, k, j, g] = push(block, block, sp=to)

    def along_group(m, k, j):
        if k == 0 and j == 0:
            return
        for g in range(1, groups):
            block = block_of(m, k, j, 0)
            got[m, k, j, g] = push(block, block, gr=lax.rem(group + g, groups))

    def along_section(m, k, j, g):
        if k == 0 and j == 0:
            return
        block = block_of(m, k, j, g)
        for t in range(1, sections):
            copy = push(block, block, tp=lax.rem(section + t, sections))
            crossed.setdefault((m, k), []).append(copy)

    def first(m, k):
        if k > 0:
            got[m, k, 0, 0].wait_recv()
        if ORDERS[m][k % len(ORDERS[m])]:
            along_group(m, k, 0)
            along_place(m, k, 0)
        else:
            along_place(m, k, 0)
            along_group(m, k, 0)
        along_section(m, k, 0, 0)
        if ORDERS[m][k % len(ORDERS[m])] and k == 0:
            second(m, k)

    def second(m, k):
        if ORDERS[m][k % len(ORDERS[m])]:
            for g in range(1, groups):
                if k > 0:
                    got[m, k, 0, g].wait_recv()
                along_place(m, k, g)
                along_section(m, k, 0, g)
        else:
            for j in range(1, inner):
                got[m, k, j, 0].wait_recv()
                along_group(m, k, j)
                along_section(m, k, j, 0)

    def third(m, k):
        if ORDERS[m][k % len(ORDERS[m])]:
            lasts = [(j, g) for j in range(1, inner) for g in range(groups)]
        else:
            lasts = [(j, g) for j in range(inner) for g in range(1, groups) if k > 0 or j > 0]
        for j, g in lasts:
            got[m, k, j, g].wait_recv()
            along_section(m, k, j, g)

    def normalise(at):
        fills[at].wait()
        step = 32

        @pl.loop(0, stage_rows // step)
        def _(i):
            here = pl.ds(pl.multiple_of(at * stage_rows + i * step, step), step)
            x = raw[here, :].astype(jnp.float32)
            mean = jnp.mean(x, axis=1, keepdims=True)
            centred = x - mean
            var = jnp.mean(centred * centred, axis=1, keepdims=True)
            scale = gain[...].astype(jnp.float32).reshape(1, width)
            normed[here, :] = (centred * lax.rsqrt(var + epsilon) * scale).astype(jnp.bfloat16)

    def multiply(m, k):
        for copy in crossed.get((m, k), ()):
            copy.wait_recv()
        span = inner * shard
        start = pl.multiple_of(lax.rem(lane + depth - k, depth) * span, span)
        out = jnp.dot(normed[:, pl.ds(start, span)], weights[m, pl.ds(start, span), :], preferred_element_type=jnp.float32)
        if k == 0:
            acc[m] = out
        else:
            acc[m] += out

    swapped = {}

    def exchange(m):
        for pair in range(seats):
            seq, head = pair // kv_heads, pair % kv_heads
            cut = slice(head * head_size, (head + 1) * head_size)
            first = acc[m, seq * sub:seq * sub + half, cut]
            second = acc[m, seq * sub + half:(seq + 1) * sub, cut]
            outgoing[m, pair] = jnp.concatenate([first, second], axis=1).astype(jnp.bfloat16)
        for i in range(1, seats):
            to = lax.rem(seat + i, seats)
            swapped[m, i] = push(outgoing.at[m, to], incoming.at[m, seat], sp=to)
        incoming[m, pl.ds(seat, 1)] = outgoing[m, pl.ds(seat, 1)]

    loads[0].wait()
    first(0, 0)
    along_lane(0)
    loads[1].wait()
    along_lane(1)
    first(1, 0)
    steps = [(NORM_AT[at], "norm", normalise, (at,)) for at in range(STAGES)]
    for m in range(2):
        end = 0.0
        for k in range(depth):
            base = m * LAG + k * LANE
            if k > 0:
                steps.append((base, "first", first, (m, k)))
            if not (k == 0 and ORDERS[m][0]):
                steps.append((base + HOP, "second", second, (m, k)))
            steps.append((base + 2 * HOP, "third", third, (m, k)))
            end = max(end, base + 2 * HOP + CROSS, NORM_AT[-1] + 0.01 * (k + 1))
            steps.append((end, "times", multiply, (m, k)))
        steps.append((end + 0.001, "trade", exchange, (m,)))
    for _, _, call, arguments in sorted(steps, key=lambda step: step[0]):
        call(*arguments)

    query = queries[...].astype(jnp.float32)
    query = jnp.concatenate([query[:, g * head_size:(g + 1) * head_size] for g in range(heads)], axis=0)
    blank = jnp.zeros_like(query)
    query = jnp.concatenate(
        [jnp.concatenate([query, blank], axis=1), jnp.concatenate([blank, query], axis=1)], axis=0
    ).astype(jnp.bfloat16)
    mine = lax.broadcasted_iota(jnp.int32, (kv_heads, heads), 0) == lax.rem(seat, kv_heads)
    shift = jnp.sum(jnp.where(mine, head_shift[...], 0.0), axis=0, keepdims=True)
    eye = lax.broadcasted_iota(jnp.int32, (heads, heads), 0) == lax.broadcasted_iota(jnp.int32, (heads, heads), 1)
    shift = jnp.sum(jnp.where(eye, jnp.broadcast_to(shift, (heads, heads)), 0.0), axis=1, keepdims=True)
    later = (
        lax.broadcasted_iota(jnp.int32, (half, half), 0) > lax.broadcasted_iota(jnp.int32, (half, half), 1)
    ).astype(jnp.float32)

    for i in range(1, seats):
        swapped[0, i].wait_recv()
    keys = incoming[0].reshape(seats * half, 2 * head_size)
    logits = lax.dot_general(query, keys, (((1,), (1,)), ((), ())), preferred_element_type=jnp.float32)
    logits = logits * head_size ** (-0.5)
    betas, keeps = [], []
    for at in range(2 * seats):
        q, h = at // 2, at % 2
        z = logits[h * heads:(h + 1) * heads, q * half:(q + 1) * half]
        z = z + shift + key_shift[:, at * half:(at + 1) * half]
        tail = jnp.log1p(jnp.exp(-jnp.abs(z)))
        betas.append(jnp.minimum(z, 0.0) - tail)
        keeps.append(jnp.minimum(-z, 0.0) - tail)
    within = jnp.dot(
        jnp.concatenate(keeps, axis=0), later, preferred_element_type=jnp.float32, precision=lax.Precision.HIGHEST
    )
    running = jnp.zeros((heads, 1), jnp.float32)
    local = [None] * (2 * seats)
    for at in reversed(range(2 * seats)):
        local[at] = jnp.exp(betas[at] + within[at * heads:(at + 1) * heads] + running)
        running = running + jnp.sum(keeps[at], axis=1, keepdims=True)
    local = jnp.concatenate(
        [jnp.concatenate(local[0::2], axis=1), jnp.concatenate(local[1::2], axis=1)], axis=0
    ).astype(jnp.bfloat16)
    totals[section] = jnp.broadcast_to(running, totals.shape[1:])
    arrivals = [
        push(totals.at[section], totals.at[section], tp=lax.rem(section + t, sections)) for t in range(1, sections)
    ]
    for copy in arrivals:
        copy.wait_recv()
    carry = jnp.zeros((heads, head_size), jnp.float32)
    for t in reversed(range(sections)):
        carry = carry + jnp.where(section < t, totals[t][:, :head_size], 0.0)
    carry = jnp.exp(carry)

    for i in range(1, seats):
        swapped[1, i].wait_recv()
    values = incoming[1].reshape(seats * half, 2 * head_size)
    part = jnp.dot(local, values, preferred_element_type=jnp.float32)
    part = carry * (part[:heads, :head_size] + part[heads:, head_size:])
    parts[section] = jnp.concatenate([part, part], axis=1)
    arrivals = [
        push(parts.at[section], parts.at[section], tp=lax.rem(section + t, sections)) for t in range(1, sections)
    ]
    for q in range(seats):
        for h in range(2):
            cut = slice(h * head_size, (h + 1) * head_size)
            start = (2 * q + h) * half
            cache[0, start:start + half, :] = jnp.concatenate([incoming[0, q][:, cut], incoming[1, q][:, cut]], axis=1)
    for copy in arrivals:
        copy.wait_recv()
    total = parts[0]
    for t in range(1, sections):
        total = total + parts[t]
    for g in range(heads):
        read[:, g * head_size:(g + 1) * head_size] = total[g:g + 1, :head_size]
    for copy in sent:
        copy.wait_send()


def hand_over(cache, read, cache_out, read_out):
    cache_out[...] = cache[...]
    read_out[...] = read[...]


def copies(grid):
    depth, inner, groups, sections = grid
    pieces = depth * inner * groups
    gather = pieces + (pieces - groups) * (sections - 1)
    return 2 * gather + 2 * (depth * inner - 1) + 2 * (sections - 1)


def local(grid, tokens, ln_gain, w_key, w_value, queries, head_shift, key_shift):
    depth, inner, groups, sections = grid
    seats = depth * inner
    seqs, _, sub, width = tokens.shape
    rows = seqs * sub
    columns = w_key.shape[1]
    kv_heads, heads = head_shift.shape
    head_size = columns // kv_heads
    vmem = pl.BlockSpec(memory_space=pltpu.VMEM)
    hbm = pl.BlockSpec(memory_space=pl.ANY)
    count = copies(grid)
    cache, read = pl.pallas_call(
        functools.partial(body, grid, head_size),
        out_shape=(
            jax.ShapeDtypeStruct((1, seats * sub, 2 * head_size), jnp.bfloat16),
            jax.ShapeDtypeStruct((1, heads * head_size), jnp.float32),
        ),
        in_specs=[hbm, vmem, hbm, hbm, vmem, vmem, vmem],
        out_specs=(vmem, vmem),
        scratch_shapes=[
            pltpu.VMEM((rows, width), jnp.bfloat16),
            pltpu.VMEM((rows, width), jnp.bfloat16),
            pltpu.VMEM((2, width, columns), jnp.bfloat16),
            pltpu.VMEM((2, rows, columns), jnp.float32),
            pltpu.VMEM((2, seats, sub // 2, 2 * head_size), jnp.bfloat16),
            pltpu.VMEM((2, seats, sub // 2, 2 * head_size), jnp.bfloat16),
            pltpu.VMEM((sections, heads, 2 * head_size), jnp.float32),
            pltpu.VMEM((sections, heads, 2 * head_size), jnp.float32),
            pltpu.SemaphoreType.DMA((count,)),
            pltpu.SemaphoreType.DMA((count,)),
            pltpu.SemaphoreType.DMA((2 + STAGES,)),
        ],
        compiler_params=pltpu.CompilerParams(
            collective_id=0, has_side_effects=True, vmem_limit_bytes=60 * 1024 * 1024
        ),
    )(tokens.reshape(rows, width), ln_gain, w_key, w_value, queries, head_shift, key_shift)
    return pl.pallas_call(
        hand_over,
        out_shape=(jax.ShapeDtypeStruct(cache.shape, cache.dtype), jax.ShapeDtypeStruct(read.shape, read.dtype)),
        in_specs=[vmem, vmem],
        out_specs=(vmem, vmem),
    )(cache, read)


def solution(mesh):
    in_specs = (
        P("gr", "tp", "sp", None),
        P(),
        P("sp", None),
        P("sp", None),
        P(("gr", "sp"), None),
        P(),
        P(("gr", "sp"), "tp"),
    )
    out_specs = (P(("gr", "sp"), "tp", None), P(("gr", "sp"), None))
    return jax.shard_map(
        functools.partial(local, layout(mesh)), mesh=mesh, in_specs=in_specs, out_specs=out_specs, check_vma=False
    )
```
